32 devices in a mesh: sp: 8 (over z, y), tp: 4 (over x, core).
Axes of the slice: x: 2, y: 2, z: 4, core: 2. Of those that a mesh axis runs over, the one named last changes fastest.
Arguments:
- query_a: bfloat16 [1536, 2048], P('sp', 'tp'), may hold values from -7.5 to 7.5
- key_a: bfloat16 [1536, 1024], P('sp', 'tp'), may hold values from -7.5 to 7.5
- value_a: bfloat16 [1536, 1024], P('sp', 'tp'), may hold values from -6 to 6
- query_b: bfloat16 [1536, 2048], P('sp', 'tp'), may hold values from -7.5 to 7.5
- key_b: bfloat16 [1536, 512], P('sp', 'tp'), may hold values from -7.5 to 7.5
- value_b: bfloat16 [1536, 512], P('sp', 'tp'), may hold values from -6 to 6
- gain_a: float32 [2, 128], replicated, may hold values from 1 to 6.5
- gain_b: float32 [2, 64], replicated, may hold values from 1 to 8.5
- out_a: bfloat16 [2048, 4096], P('tp'), may hold values from -0.5 to 0.5
- out_b: bfloat16 [2048, 4096], P('tp'), may hold values from -0.5 to 0.5
- residual: bfloat16 [1536, 4096], P('sp'), may hold values from -6 to 6
- norm_gain: float32 [4096], replicated, may hold values from 0.1 to 1.9
- gate_weight: bfloat16 [4096, 6144], P('sp', 'tp'), may hold values from -0.09375 to 0.09375
- up_weight: bfloat16 [4096, 6144], P('sp', 'tp'), may hold values from -0.09375 to 0.09375
- down_weight: bfloat16 [6144, 4096], P('tp', 'sp'), may hold values from -0.3125 to 0.3125
Outputs:
- output: bfloat16 [1536, 4096], P(('sp', 'tp'))
The draws below stay inside these ranges and needn't reach their ends.
All inputs are finite; a program needn't handle non-finite values.
Results may differ from the reference program's by a relative error of at most 0.017.
The reference program's roundings to bfloat16 on the way count: a program that leaves them out, or rounds other values in their place, can miss the bound.
Values may be sent and summed in bfloat16 or wider, within the bound.
A program may use at most 128 MiB of HBM per device.

```python
import math
import jax
import jax.numpy as jnp
from jax import lax

HEAD_A = 128
HEAD_B = 64
HEADS_A = 16
KV_A = 8
HEADS_B = 32
KV_B = 8
FF = 6144
GRID_W = 64
D = 4096
TOKENS = 1536
N_TP = 4


def plant_pairs(key, query_heads, kv_heads, head_size):
    keys_split = jax.random.split(key, 2)
    queries = jax.random.normal(keys_split[0], (TOKENS, query_heads * head_size), jnp.float32)
    key_rows = jax.random.normal(keys_split[1], (TOKENS, kv_heads * head_size), jnp.float32)
    return (jnp.clip(queries, -7.5, 7.5), jnp.clip(key_rows, -7.5, 7.5))


def draw_query_a(key, part):
    return plant_pairs(jax.random.fold_in(key, 11), HEADS_A, KV_A, HEAD_A)[0].astype(jnp.bfloat16)


def draw_key_a(key, part):
    return plant_pairs(jax.random.fold_in(key, 11), HEADS_A, KV_A, HEAD_A)[1].astype(jnp.bfloat16)


def draw_query_b(key, part):
    return plant_pairs(jax.random.fold_in(key, 12), HEADS_B, KV_B, HEAD_B)[0].astype(jnp.bfloat16)


def draw_key_b(key, part):
    return plant_pairs(jax.random.fold_in(key, 12), HEADS_B, KV_B, HEAD_B)[1].astype(jnp.bfloat16)


def draw_gain_a(key, part):
    return jax.random.uniform(jax.random.fold_in(key, 21), (2, HEAD_A), jnp.float32, 1.0, 2.0)


def draw_gain_b(key, part):
    return jax.random.uniform(jax.random.fold_in(key, 22), (2, HEAD_B), jnp.float32, 1.0, 2.0)


def block_scale(rng, shape, cuts, smallest, largest):
    def one(dim, shards_of):
        draws = jax.random.uniform(jax.random.fold_in(jax.random.fold_in(rng, 6), dim), (shards_of,), jnp.float32, smallest / len(cuts), largest / len(cuts))
        return jnp.repeat(jnp.exp(draws), shape[dim] // shards_of).reshape((-1,) + (1,) * (len(shape) - dim - 1))

    factor_of = one(*cuts[0])
    for cut in cuts[1:]:
        factor_of = factor_of * one(*cut)
    return factor_of


def bell_draw(stream_key, shape, width, bound, cuts=(), kind=jnp.bfloat16):
    values = jax.random.normal(stream_key, shape, jnp.float32) * width
    if len(cuts) > 0:
        values = block_scale(stream_key, shape, cuts, -0.22, 0.18) * values
    return jnp.clip(values, min=-bound, max=bound).astype(kind)


def setup_inputs(seed: int = 0) -> dict:
    key_list = jax.random.split(jax.random.key(seed), 16)
    return {
        "query_a": draw_query_a(jax.random.fold_in(key_list[15], 71), 0),
        "key_a": draw_key_a(jax.random.fold_in(key_list[15], 71), 0),
        "value_a": bell_draw(key_list[2], (TOKENS, KV_A * HEAD_A), 1.0, 6.0, ((0, 8), (1, 4))),
        "query_b": draw_query_b(jax.random.fold_in(key_list[15], 71), 0),
        "key_b": draw_key_b(jax.random.fold_in(key_list[15], 71), 0),
        "value_b": bell_draw(key_list[5], (TOKENS, KV_B * HEAD_B), 1.0, 6.0, ((0, 8), (1, 4))),
        "gain_a": draw_gain_a(jax.random.fold_in(key_list[15], 71), 0),
        "gain_b": draw_gain_b(jax.random.fold_in(key_list[15], 71), 0),
        "out_a": bell_draw(key_list[8], (HEADS_A * HEAD_A, D), (D // 25) ** -0.5, 0.5, ((0, 4),)),
        "out_b": bell_draw(key_list[9], (HEADS_B * HEAD_B, D), (D // 25) ** -0.5, 0.5, ((0, 4),)),
        "residual": bell_draw(key_list[10], (TOKENS, D), 1.0, 6.0, ((0, 8),)),
        "norm_gain": jnp.clip(1.0 + 0.18 * jax.random.normal(key_list[11], (D,), jnp.float32), 0.1, 1.9),
        "gate_weight": bell_draw(key_list[12], (D, FF), D ** -0.5, 0.09375, ((0, 8), (1, 4))),
        "up_weight": bell_draw(key_list[13], (D, FF), D ** -0.5, 0.09375, ((0, 8), (1, 4))),
        "down_weight": bell_draw(key_list[14], (FF, D), (FF // 16) ** -0.5, 0.3125, ((0, 4), (1, 8))),
    }


epsilon = 1e-06
theta_base = 10000.0

def rotate(inputs, num_heads, head_size, first_pos, gain):
    tok_rows = inputs.shape[0]
    vectors = inputs.astype(jnp.float32).reshape(tok_rows, num_heads, head_size)
    vectors = vectors * lax.rsqrt(lax.optimization_barrier(jnp.mean(vectors * vectors, axis=-1, keepdims=True)) + epsilon) * gain
    position = first_pos + jnp.arange(tok_rows, dtype=jnp.int32)
    grid_row = (position // GRID_W).astype(jnp.float32)
    grid_col = (position % GRID_W).astype(jnp.float32)
    quarter = head_size // 4
    inv_freq = theta_base ** (-4.0 * jnp.arange(quarter, dtype=jnp.float32) / head_size)
    angle_row = grid_row[:, None] * inv_freq[None, :]
    angle_col = grid_col[:, None] * inv_freq[None, :]
    angles = jnp.concatenate([angle_row, angle_row, angle_col, angle_col], axis=-1)
    quarters = vectors.reshape(tok_rows, num_heads, 4, quarter)
    rotated = jnp.stack([-quarters[:, :, 1], quarters[:, :, 0], -quarters[:, :, 3], quarters[:, :, 2]], axis=2)
    rotated = rotated.reshape(tok_rows, num_heads, head_size)
    result = vectors * jnp.cos(angles)[:, None, :] + rotated * jnp.sin(angles)[:, None, :]
    return result.reshape(tok_rows, num_heads * head_size).astype(jnp.bfloat16)

def attend_all(queries, key_rows, values, num_heads, kv_heads, head_size):
    tokens_all = queries.shape[0]
    block_len = math.gcd(tokens_all, 512)
    groups = num_heads // kv_heads
    k_heads = key_rows.astype(jnp.float32).reshape(tokens_all, kv_heads, head_size)
    v_heads = values.astype(jnp.float32).reshape(tokens_all, kv_heads, head_size)

    def one_block(q_block):
        q_heads = q_block.astype(jnp.float32).reshape(block_len, kv_heads, groups, head_size)
        scores = jnp.einsum('tkgd,pkd->kgtp', q_heads, k_heads) * head_size ** (-0.5)
        row_max = lax.optimization_barrier(jnp.max(scores, axis=-1, keepdims=True))
        exp_scores = jnp.exp(scores - row_max)
        rounded = lax.optimization_barrier(exp_scores.astype(jnp.bfloat16)).astype(jnp.float32)
        blended = jnp.einsum('kgtp,pkd->kgtd', rounded, v_heads) / lax.optimization_barrier(jnp.sum(exp_scores, axis=-1))[..., None]
        return blended.transpose(2, 0, 1, 3).reshape(block_len, num_heads * head_size).astype(jnp.bfloat16)
    blocks = queries.reshape(tokens_all // block_len, block_len, num_heads * head_size)
    return lax.map(one_block, blocks).reshape(tokens_all, num_heads * head_size)

def normalize(mixed_rows, gain):
    scale = lax.rsqrt(lax.optimization_barrier(jnp.mean(mixed_rows * mixed_rows, axis=-1, keepdims=True)) + epsilon)
    return (mixed_rows * scale * gain).astype(jnp.bfloat16)

def reference(query_a, key_a, value_a, query_b, key_b, value_b, gain_a, gain_b, out_a, out_b, residual, norm_gain, gate_weight, up_weight, down_weight):
    turned_qa = rotate(query_a, HEADS_A, HEAD_A, 0, gain_a[0])
    turned_ka = rotate(key_a, KV_A, HEAD_A, 0, gain_a[1])
    turned_qb = rotate(query_b, HEADS_B, HEAD_B, 0, gain_b[0])
    turned_kb = rotate(key_b, KV_B, HEAD_B, 0, gain_b[1])
    attn_a = attend_all(turned_qa, turned_ka, value_a, HEADS_A, KV_A, HEAD_A)
    attn_b = attend_all(turned_qb, turned_kb, value_b, HEADS_B, KV_B, HEAD_B)
    cols_a = HEADS_A * HEAD_A // N_TP
    cols_b = HEADS_B * HEAD_B // N_TP
    head_sum = jnp.zeros((TOKENS, D), jnp.float32)
    for block_num in range(N_TP):
        part_a = jnp.dot(attn_a[:, block_num * cols_a:(block_num + 1) * cols_a], out_a[block_num * cols_a:(block_num + 1) * cols_a], preferred_element_type=jnp.float32)
        part_b = jnp.dot(attn_b[:, block_num * cols_b:(block_num + 1) * cols_b], out_b[block_num * cols_b:(block_num + 1) * cols_b], preferred_element_type=jnp.float32)
        head_sum = head_sum + lax.optimization_barrier((part_a + part_b).astype(jnp.bfloat16)).astype(jnp.float32)
    mixed_rows = residual.astype(jnp.float32) + head_sum
    normed = normalize(mixed_rows, norm_gain)
    gate_act = jnp.dot(normed, gate_weight, preferred_element_type=jnp.float32)
    up_act = jnp.dot(normed, up_weight, preferred_element_type=jnp.float32)
    hidden = (jax.nn.silu(gate_act) * up_act).astype(jnp.bfloat16)
    unit_block = FF // N_TP
    branch_sum = jnp.zeros((TOKENS, D), jnp.float32)
    for block_num in range(N_TP):
        part_down = jnp.dot(hidden[:, block_num * unit_block:(block_num + 1) * unit_block], down_weight[block_num * unit_block:(block_num + 1) * unit_block], preferred_element_type=jnp.float32)
        branch_sum = branch_sum + lax.optimization_barrier(part_down.astype(jnp.bfloat16)).astype(jnp.float32)
    return (mixed_rows + 0.5 * branch_sum).astype(jnp.bfloat16)
```

```python
import jax
import jax.numpy as jnp
from jax import lax
from jax.sharding import PartitionSpec as P

HEAD_A = 128
HEAD_B = 64
GRID_W = 64


epsilon = 1e-06
theta_base = 10000.0


def rotate(inputs, num_heads, head_size, first_pos, gain):
    tok_rows = inputs.shape[0]
    vectors = inputs.astype(jnp.float32).reshape(tok_rows, num_heads, head_size)
    vectors = (
        vectors * lax.rsqrt(jnp.mean(vectors * vectors, axis=-1, keepdims=True) + epsilon) * gain
    )
    position = first_pos + jnp.arange(tok_rows, dtype=jnp.int32)
    grid_row = (position // GRID_W).astype(jnp.float32)
    grid_col = (position % GRID_W).astype(jnp.float32)
    quarter = head_size // 4
    inv_freq = theta_base ** (-4.0 * jnp.arange(quarter, dtype=jnp.float32) / head_size)
    angle_row = grid_row[:, None] * inv_freq[None, :]
    angle_col = grid_col[:, None] * inv_freq[None, :]
    angles = jnp.concatenate([angle_row, angle_row, angle_col, angle_col], axis=-1)
    quarters = vectors.reshape(tok_rows, num_heads, 4, quarter)
    rotated = jnp.stack(
        [-quarters[:, :, 1], quarters[:, :, 0], -quarters[:, :, 3], quarters[:, :, 2]], axis=2
    )
    rotated = rotated.reshape(tok_rows, num_heads, head_size)
    result = vectors * jnp.cos(angles)[:, None, :] + rotated * jnp.sin(angles)[:, None, :]
    return result.reshape(tok_rows, num_heads * head_size).astype(jnp.bfloat16)


def start_state(kv_heads, groups, tok_rows, head_size):
    return (
        jnp.full((kv_heads, groups, tok_rows), -1e30, jnp.float32),
        jnp.zeros((kv_heads, groups, tok_rows), jnp.float32),
        jnp.zeros((kv_heads, groups, tok_rows, head_size), jnp.float32),
    )


def attend(state, queries, key_rows, values, head_size):
    run_max, run_sum, run_acc = state
    kv_heads = key_rows.shape[1] // head_size
    groups = run_max.shape[1]
    q_heads = queries.reshape(queries.shape[0], kv_heads, groups, head_size)
    k_heads = key_rows.reshape(key_rows.shape[0], kv_heads, head_size)
    v_heads = values.reshape(values.shape[0], kv_heads, head_size)
    scores = jnp.einsum(
        "tkgd,pkd->kgtp", q_heads, k_heads, preferred_element_type=jnp.float32
    ) * head_size ** (-0.5)
    new_max = jnp.maximum(run_max, jnp.max(scores, axis=-1))
    exp_scores = jnp.exp(scores - new_max[..., None])
    new_sum = jnp.sum(exp_scores, axis=-1)
    new_acc = jnp.einsum(
        "kgtp,pkd->kgtd",
        exp_scores.astype(jnp.bfloat16),
        v_heads,
        preferred_element_type=jnp.float32,
    )
    return (new_max, new_sum, new_acc)


def finish(state, num_cols):
    blended = state[2] / state[1][..., None]
    return blended.transpose(2, 0, 1, 3).reshape(blended.shape[2], num_cols).astype(jnp.bfloat16)


def normalize(mixed_rows, gain):
    scale = lax.rsqrt(jnp.mean(mixed_rows * mixed_rows, axis=-1, keepdims=True) + epsilon)
    return (mixed_rows * scale * gain).astype(jnp.bfloat16)


def on_device(
    query_a,
    key_a,
    value_a,
    query_b,
    key_b,
    value_b,
    gain_a,
    gain_b,
    out_a,
    out_b,
    residual,
    norm_gain,
    gate_weight,
    up_weight,
    down_weight,
):
    tok_rows = query_a.shape[0]
    first_pos = lax.axis_index("sp") * tok_rows
    heads_a = query_a.shape[1] // HEAD_A
    heads_b = query_b.shape[1] // HEAD_B
    kv_heads_a = key_a.shape[1] // HEAD_A
    kv_heads_b = key_b.shape[1] // HEAD_B
    kv_width_b = kv_heads_b * HEAD_B
    turned_qa = rotate(query_a, heads_a, HEAD_A, first_pos, gain_a[0])
    turned_ka = rotate(key_a, kv_heads_a, HEAD_A, first_pos, gain_a[1])
    turned_qb = rotate(query_b, heads_b, HEAD_B, first_pos, gain_b[0])
    turned_kb = rotate(key_b, kv_heads_b, HEAD_B, first_pos, gain_b[1])
    widths = (key_a.shape[1], value_a.shape[1], key_b.shape[1], value_b.shape[1])
    cuts = [sum(widths[:i]) for i in range(5)]
    sp = lax.axis_size("sp")
    tp = lax.axis_size("tp")
    ff_own = gate_weight.shape[1] // sp
    both = jnp.concatenate(
        [
            gate_weight.reshape(gate_weight.shape[0], sp, ff_own),
            up_weight.reshape(up_weight.shape[0], sp, ff_own),
        ],
        axis=2,
    ).transpose(1, 0, 2)
    both = lax.all_to_all(both, "sp", 0, 0, tiled=True).reshape(-1, 2 * ff_own)
    pairs = lax.all_gather(
        jnp.concatenate([turned_ka, value_a, turned_kb, value_b], axis=1), "sp", axis=0, tiled=True
    )
    initial = (
        start_state(kv_heads_a, heads_a // kv_heads_a, tok_rows, HEAD_A),
        start_state(kv_heads_b, heads_b // kv_heads_b, tok_rows, HEAD_B),
    )
    pieces = [pairs[:, cuts[i] : cuts[i + 1]] for i in range(4)]
    state_a = attend(initial[0], turned_qa, pieces[0], pieces[1], HEAD_A)
    state_b = attend(initial[1], turned_qb, pieces[2], pieces[3], HEAD_B)
    attn_a = finish(state_a, query_a.shape[1])
    attn_b = finish(state_b, query_b.shape[1])
    own_rows = tok_rows // tp
    own_start = lax.axis_index("tp") * own_rows
    head_sum = lax.psum_scatter(
        (
            jnp.dot(attn_a, out_a, preferred_element_type=jnp.float32)
            + jnp.dot(attn_b, out_b, preferred_element_type=jnp.float32)
        ).astype(jnp.bfloat16),
        "tp",
        scatter_dimension=0,
        tiled=True,
    ).astype(jnp.float32)
    mixed_rows = (
        lax.dynamic_slice_in_dim(residual, own_start, own_rows, 0).astype(jnp.float32) + head_sum
    )
    normed = lax.all_gather(normalize(mixed_rows, norm_gain), ("sp", "tp"), axis=0, tiled=True)
    acts = jnp.dot(normed, both, preferred_element_type=jnp.float32)
    hidden = (jax.nn.silu(acts[:, :ff_own]) * acts[:, ff_own:]).astype(jnp.bfloat16)
    hidden = lax.all_gather(hidden, "sp", axis=0)
    down_rows = down_weight.reshape(sp, ff_own, down_weight.shape[1])
    down_all = jnp.einsum("smk,skn->mn", hidden, down_rows, preferred_element_type=jnp.float32)
    cols = down_weight.shape[1]
    branch = lax.psum_scatter(
        down_all.astype(jnp.bfloat16).reshape(sp, tp, own_rows, cols).transpose(1, 0, 2, 3),
        "tp",
        scatter_dimension=0,
        tiled=True,
    ).reshape(sp, own_rows, cols)
    branch_sum = lax.all_to_all(branch, "sp", 0, 0, tiled=True).transpose(1, 0, 2)
    branch_sum = branch_sum.reshape(own_rows, sp * cols).astype(jnp.float32)
    return (mixed_rows + 0.5 * branch_sum).astype(jnp.bfloat16)


def solution(mesh):
    return jax.shard_map(
        on_device,
        mesh=mesh,
        in_specs=(
            P("sp", "tp"),
            P("sp", "tp"),
            P("sp", "tp"),
            P("sp", "tp"),
            P("sp", "tp"),
            P("sp", "tp"),
            P(),
            P(),
            P("tp", None),
            P("tp", None),
            P("sp", None),
            P(),
            P("sp", "tp"),
            P("sp", "tp"),
            P("tp", "sp"),
        ),
        out_specs=P(("sp", "tp"), None),
        check_vma=False,
    )
```

```python
import jax
import jax.numpy as jnp
from jax import lax
from jax.sharding import PartitionSpec as P

HEAD_A = 128
HEAD_B = 64
GRID_W = 64


epsilon = 1e-06
theta_base = 10000.0


def rotate(inputs, num_heads, head_size, first_pos, gain):
    tok_rows = inputs.shape[0]
    vectors = inputs.astype(jnp.float32).reshape(tok_rows, num_heads, head_size)
    vectors = (
        vectors * lax.rsqrt(jnp.mean(vectors * vectors, axis=-1, keepdims=True) + epsilon) * gain
    )
    position = first_pos + jnp.arange(tok_rows, dtype=jnp.int32)
    grid_row = (position // GRID_W).astype(jnp.float32)
    grid_col = (position % GRID_W).astype(jnp.float32)
    quarter = head_size // 4
    inv_freq = theta_base ** (-4.0 * jnp.arange(quarter, dtype=jnp.float32) / head_size)
    angle_row = grid_row[:, None] * inv_freq[None, :]
    angle_col = grid_col[:, None] * inv_freq[None, :]
    angles = jnp.concatenate([angle_row, angle_row, angle_col, angle_col], axis=-1)
    quarters = vectors.reshape(tok_rows, num_heads, 4, quarter)
    rotated = jnp.stack(
        [-quarters[:, :, 1], quarters[:, :, 0], -quarters[:, :, 3], quarters[:, :, 2]], axis=2
    )
    rotated = rotated.reshape(tok_rows, num_heads, head_size)
    result = vectors * jnp.cos(angles)[:, None, :] + rotated * jnp.sin(angles)[:, None, :]
    return result.reshape(tok_rows, num_heads * head_size).astype(jnp.bfloat16)


def start_state(kv_heads, groups, tok_rows, head_size):
    return (
        jnp.full((kv_heads, groups, tok_rows), -1e30, jnp.float32),
        jnp.zeros((kv_heads, groups, tok_rows), jnp.float32),
        jnp.zeros((kv_heads, groups, tok_rows, head_size), jnp.float32),
    )


def attend(state, queries, key_rows, values, head_size):
    run_max, run_sum, run_acc = state
    kv_heads = key_rows.shape[1] // head_size
    groups = run_max.shape[1]
    q_heads = queries.reshape(queries.shape[0], kv_heads, groups, head_size)
    k_heads = key_rows.reshape(key_rows.shape[0], kv_heads, head_size)
    v_heads = values.reshape(values.shape[0], kv_heads, head_size)
    scores = jnp.einsum(
        "tkgd,pkd->kgtp", q_heads, k_heads, preferred_element_type=jnp.float32
    ) * head_size ** (-0.5)
    new_max = jnp.maximum(run_max, jnp.max(scores, axis=-1))
    exp_scores = jnp.exp(scores - new_max[..., None])
    new_sum = jnp.sum(exp_scores, axis=-1)
    new_acc = jnp.einsum(
        "kgtp,pkd->kgtd",
        exp_scores.astype(jnp.bfloat16),
        v_heads,
        preferred_element_type=jnp.float32,
    )
    return (new_max, new_sum, new_acc)


def finish(state, num_cols):
    blended = state[2] / state[1][..., None]
    return blended.transpose(2, 0, 1, 3).reshape(blended.shape[2], num_cols).astype(jnp.bfloat16)


def normalize(mixed_rows, gain):
    scale = lax.rsqrt(jnp.mean(mixed_rows * mixed_rows, axis=-1, keepdims=True) + epsilon)
    return (mixed_rows * scale * gain).astype(jnp.bfloat16)


def on_device(
    query_a,
    key_a,
    value_a,
    query_b,
    key_b,
    value_b,
    gain_a,
    gain_b,
    out_a,
    out_b,
    residual,
    norm_gain,
    gate_weight,
    up_weight,
    down_weight,
):
    tok_rows = query_a.shape[0]
    first_pos = lax.axis_index("sp") * tok_rows
    heads_a = query_a.shape[1] // HEAD_A
    heads_b = query_b.shape[1] // HEAD_B
    kv_heads_a = key_a.shape[1] // HEAD_A
    kv_heads_b = key_b.shape[1] // HEAD_B
    kv_width_b = kv_heads_b * HEAD_B
    turned_qa = rotate(query_a, heads_a, HEAD_A, first_pos, gain_a[0])
    turned_ka = rotate(key_a, kv_heads_a, HEAD_A, first_pos, gain_a[1])
    turned_qb = rotate(query_b, heads_b, HEAD_B, first_pos, gain_b[0])
    turned_kb = rotate(key_b, kv_heads_b, HEAD_B, first_pos, gain_b[1])
    widths = (key_a.shape[1], value_a.shape[1], key_b.shape[1], value_b.shape[1])
    cuts = [sum(widths[:i]) for i in range(5)]
    sp = lax.axis_size("sp")
    tp = lax.axis_size("tp")
    ff_own = gate_weight.shape[1] // sp
    both = jnp.concatenate(
        [
            gate_weight.reshape(gate_weight.shape[0], sp, ff_own),
            up_weight.reshape(up_weight.shape[0], sp, ff_own),
        ],
        axis=2,
    ).transpose(1, 0, 2)
    both = lax.all_to_all(both, "sp", 0, 0, tiled=True).reshape(-1, 2 * ff_own)
    pairs = lax.all_gather(
        jnp.concatenate([turned_ka, value_a, turned_kb, value_b], axis=1), "sp", axis=0, tiled=True
    )
    initial = (
        start_state(kv_heads_a, heads_a // kv_heads_a, tok_rows, HEAD_A),
        start_state(kv_heads_b, heads_b // kv_heads_b, tok_rows, HEAD_B),
    )
    pieces = [pairs[:, cuts[i] : cuts[i + 1]] for i in range(4)]
    state_a = attend(initial[0], turned_qa, pieces[0], pieces[1], HEAD_A)
    state_b = attend(initial[1], turned_qb, pieces[2], pieces[3], HEAD_B)
    attn_a = finish(state_a, query_a.shape[1])
    attn_b = finish(state_b, query_b.shape[1])
    own_rows = tok_rows // tp
    own_start = lax.axis_index("tp") * own_rows
    head_sum = lax.psum_scatter(
        (
            jnp.dot(attn_a, out_a, preferred_element_type=jnp.float32)
            + jnp.dot(attn_b, out_b, preferred_element_type=jnp.float32)
        ).astype(jnp.bfloat16),
        "tp",
        scatter_dimension=0,
        tiled=True,
    ).astype(jnp.float32)
    mixed_rows = (
        lax.dynamic_slice_in_dim(residual, own_start, own_rows, 0).astype(jnp.float32) + head_sum
    )
    normed = lax.all_gather(normalize(mixed_rows, norm_gain), ("sp", "tp"), axis=0, tiled=True)
    acts = lax.dot_general(
        both, normed, (((0,), (1,)), ((), ())), preferred_element_type=jnp.float32
    )
    hidden = (jax.nn.silu(acts[:ff_own]) * acts[ff_own:]).astype(jnp.bfloat16)
    down_all = lax.dot_general(
        lax.all_gather(hidden, "sp", axis=0, tiled=True),
        down_weight,
        (((0,), (0,)), ((), ())),
        preferred_element_type=jnp.float32,
    )
    cols = down_weight.shape[1]
    branch = lax.psum_scatter(
        down_all.astype(jnp.bfloat16).reshape(sp, tp, own_rows, cols).transpose(1, 0, 2, 3),
        "tp",
        scatter_dimension=0,
        tiled=True,
    ).reshape(sp, own_rows, cols)
    branch_sum = lax.all_to_all(branch, "sp", 0, 0, tiled=True).transpose(1, 0, 2)
    branch_sum = branch_sum.reshape(own_rows, sp * cols).astype(jnp.float32)
    return (mixed_rows + 0.5 * branch_sum).astype(jnp.bfloat16)


def solution(mesh):
    return jax.shard_map(
        on_device,
        mesh=mesh,
        in_specs=(
            P("sp", "tp"),
            P("sp", "tp"),
            P("sp", "tp"),
            P("sp", "tp"),
            P("sp", "tp"),
            P("sp", "tp"),
            P(),
            P(),
            P("tp", None),
            P("tp", None),
            P("sp", None),
            P(),
            P("sp", "tp"),
            P("sp", "tp"),
            P("tp", "sp"),
        ),
        out_specs=P(("sp", "tp"), None),
        check_vma=False,
    )
```
